32 devices in a mesh: sp: 4 (over z), fs: 4 (over y, x), tp: 2 (over core).
Axes of the slice: x: 2, y: 2, z: 4, core: 2. Of those that a mesh axis runs over, the one named last changes fastest.
Arguments:
- tokens: bfloat16 [4, 768, 2048], P('fs', 'sp', 'tp'), may hold values from -24 to 24
- norm_gain: bfloat16 [2048], P('tp'), may hold values from 0.099609375 to 1.8984375
- w_q_down: bfloat16 [2048, 512], P('fs'), may hold values from -0.151 to 0.151
- q_gain: float32 [512], replicated, may hold values from 0.1 to 1.9
- w_q_nope: bfloat16 [512, 2048], P(None, 'tp'), may hold values from -1.21 to 1.21
- w_q_rope: bfloat16 [512, 1024], P(None, 'tp'), may hold values from -0.75 to 0.75
- w_kv_down: bfloat16 [2048, 256], P('fs'), may hold values from -0.151 to 0.151
- kv_gain: float32 [256], replicated, may hold values from 0.1 to 1.9
- w_k_up: bfloat16 [256, 2048], P(None, 'tp'), may hold values from -0.81 to 0.81
- w_v_up: bfloat16 [256, 2048], P(None, 'tp'), may hold values from -0.375 to 0.375
- w_k_rope: bfloat16 [2048, 64], replicated, may hold values from -0.125 to 0.125
- w_pool_in: bfloat16 [2048, 1024], P(None, 'tp'), may hold values from -0.125 to 0.125
- w_pool_mix: bfloat16 [4, 256, 256], replicated, may hold values from -0.375 to 0.375
- w_out_attn: bfloat16 [2048, 2048], P('tp'), may hold values from -0.125 to 0.125
- w_out_pool: bfloat16 [1024, 2048], P('tp'), may hold values from -0.1875 to 0.1875
Outputs:
- mixed: bfloat16 [4, 768, 2048], P('fs', ('sp', 'tp'))
The draws below stay inside these ranges and needn't reach their ends.
All inputs are finite; a program needn't handle non-finite values.
Results may differ from the reference program's by a relative error of at most 0.02.
Values may be sent and summed in bfloat16 or wider, within the bound.
No kernel may reach another device: no remote copies, remote signals or barrier semaphores. Data moves between devices by JAX's collectives and lax.ppermute only.
A program may use at most 128 MiB of HBM per device.

```python
import jax
import jax.numpy as jnp
from jax import lax

D_MODEL = 2048
HEADS = 16
NOPE_DIM = 128
ROPE_DIM = 64
VALUE_DIM = 128
Q_RANK = 512
KV_RANK = 256
POOL_CH = 1024
GRID_W = 64
TOK_DEV = 192
POOL_GROUP = 256
SEQS = 4
SEQ_LEN = 768


def draw_tokens(key, part):
    base = jax.random.normal(jax.random.fold_in(key, 11), (SEQS, SEQ_LEN, D_MODEL), jnp.float32)
    return jnp.clip(base, -6.0, 6.0).astype(jnp.bfloat16)


def draw_w_q_down(key, part):
    base = jax.random.normal(jax.random.fold_in(key, 21), (D_MODEL, Q_RANK), jnp.float32)
    base = jnp.clip(base, -6.0, 6.0) * D_MODEL ** (-0.5)
    return jnp.clip(base, -0.15, 0.15).astype(jnp.bfloat16)


def draw_w_kv_down(key, part):
    base = jax.random.normal(jax.random.fold_in(key, 31), (D_MODEL, KV_RANK), jnp.float32)
    base = jnp.clip(base, -6.0, 6.0) * D_MODEL ** (-0.5)
    return jnp.clip(base, -0.15, 0.15).astype(jnp.bfloat16)


def draw_w_q_nope(key, part):
    base = jax.random.normal(jax.random.fold_in(key, 41), (Q_RANK, HEADS * NOPE_DIM), jnp.float32)
    base = jnp.clip(base, -6.0, 6.0) * (Q_RANK // 9) ** (-0.5)
    return jnp.clip(base, -1.2, 1.2).astype(jnp.bfloat16)


def draw_w_k_up(key, part):
    base = jax.random.normal(jax.random.fold_in(key, 51), (KV_RANK, HEADS * NOPE_DIM), jnp.float32)
    base = jnp.clip(base, -6.0, 6.0) * KV_RANK ** (-0.5)
    return jnp.clip(base, -0.8, 0.8).astype(jnp.bfloat16)


def block_levels(rng, dims, cuts, least, high):
    def one(axis_at, parts):
        heights = jax.random.uniform(jax.random.fold_in(jax.random.fold_in(rng, 6), axis_at), (parts,), jnp.float32, least / len(cuts), high / len(cuts))
        return jnp.repeat(jnp.exp(heights), dims[axis_at] // parts).reshape((-1,) + (1,) * (len(dims) - axis_at - 1))

    level = one(*cuts[0])
    for cut in cuts[1:]:
        level = level * one(*cut)
    return level


def scatter_about(own_key, shape, scale, reach, cuts=(), kind=jnp.bfloat16):
    values = scale * jax.random.normal(own_key, shape, jnp.float32)
    if cuts:
        values = values * block_levels(own_key, shape, cuts, -0.22, 0.18)
    return jnp.clip(values, -reach, reach).astype(kind)


def setup_inputs(seed: int = 0) -> dict:
    arg_keys = jax.random.split(jax.random.key(seed), 16)
    return {
        "tokens": draw_tokens(jax.random.fold_in(arg_keys[15], 71), 0),
        "norm_gain": jnp.clip(1.0 + 0.18 * jax.random.normal(arg_keys[1], (D_MODEL,), jnp.float32), 0.099609375, 1.8984375).astype(jnp.bfloat16),
        "w_q_down": draw_w_q_down(jax.random.fold_in(arg_keys[15], 71), 0),
        "q_gain": jnp.clip(1.0 + 0.18 * jax.random.normal(arg_keys[3], (Q_RANK,), jnp.float32), 0.1, 1.9),
        "w_q_nope": draw_w_q_nope(jax.random.fold_in(arg_keys[15], 71), 0),
        "w_q_rope": scatter_about(arg_keys[5], (Q_RANK, HEADS * ROPE_DIM), (Q_RANK // 9) ** -0.5, 0.75, ((1, 2),)),
        "w_kv_down": draw_w_kv_down(jax.random.fold_in(arg_keys[15], 71), 0),
        "kv_gain": jnp.clip(1.0 + 0.18 * jax.random.normal(arg_keys[7], (KV_RANK,), jnp.float32), 0.1, 1.9),
        "w_k_up": draw_w_k_up(jax.random.fold_in(arg_keys[15], 71), 0),
        "w_v_up": scatter_about(arg_keys[9], (KV_RANK, HEADS * VALUE_DIM), KV_RANK ** -0.5, 0.375, ((1, 2),)),
        "w_k_rope": scatter_about(arg_keys[10], (D_MODEL, ROPE_DIM), D_MODEL ** -0.5, 0.125),
        "w_pool_in": scatter_about(arg_keys[11], (D_MODEL, POOL_CH), D_MODEL ** -0.5, 0.125, ((1, 2),)),
        "w_pool_mix": scatter_about(arg_keys[12], (4, POOL_GROUP, POOL_GROUP), POOL_GROUP ** -0.5, 0.375),
        "w_out_attn": scatter_about(arg_keys[13], (HEADS * VALUE_DIM, D_MODEL), (HEADS * VALUE_DIM) ** -0.5, 0.125, ((0, 2),)),
        "w_out_pool": scatter_about(arg_keys[14], (POOL_CH, D_MODEL), POOL_CH ** -0.5, 0.1875, ((0, 2),)),
    }


EPS = 1e-06
THETA = 10000.0
window_sizes = (2, 4, 8, 16)

def normed(values, gain_vec):
    widened = values.astype(jnp.float32)
    scaled = widened * lax.rsqrt(lax.optimization_barrier(jnp.mean(widened * widened, axis=-1, keepdims=True)) + EPS)
    return (scaled * gain_vec.astype(jnp.float32)).astype(jnp.bfloat16)

def angles(position):
    row_index = (position // GRID_W).astype(jnp.float32)
    column = (position % GRID_W).astype(jnp.float32)
    inverse = THETA ** (-jnp.arange(0, ROPE_DIM // 2, 2).astype(jnp.float32) / (ROPE_DIM // 2))
    return jnp.stack([row_index, column], axis=-1)[:, :, None] * inverse

def rotate(values, angle_table):
    full_shape = values.shape
    split_parts = values.astype(jnp.float32).reshape(full_shape[:-1] + (2, 2, ROPE_DIM // 4))
    front_half = split_parts[..., 0, :]
    back_half = split_parts[..., 1, :]
    cosine = jnp.cos(angle_table)
    sine_part = jnp.sin(angle_table)
    turned = jnp.stack([front_half * cosine - back_half * sine_part, front_half * sine_part + back_half * cosine], axis=-2)
    return turned.reshape(full_shape).astype(jnp.bfloat16)

def attend(query_nope, query_rope, key_nope, key_rope, values_all):
    length = query_nope.shape[0]
    key_wide = key_nope.astype(jnp.float32)
    rope_wide = key_rope.astype(jnp.float32)
    value_wide = values_all.astype(jnp.float32)
    score_scale = (NOPE_DIM + ROPE_DIM) ** (-0.5)

    def one_block(block):
        query_part, rope_part = block
        scores = jnp.einsum('qhd,khd->hqk', query_part.astype(jnp.float32), key_wide)
        scores = scores + jnp.einsum('qhr,kr->hqk', rope_part.astype(jnp.float32), rope_wide)
        scores = scores * score_scale
        row_max = lax.optimization_barrier(jnp.max(scores, axis=-1, keepdims=True))
        weights = jnp.exp(scores - row_max)
        row_total = lax.optimization_barrier(jnp.sum(weights, axis=-1))
        rounded = lax.optimization_barrier(weights.astype(jnp.bfloat16))
        summed = jnp.einsum('hqk,khd->qhd', rounded.astype(jnp.float32), value_wide)
        return (summed / jnp.transpose(row_total)[:, :, None]).astype(jnp.bfloat16)
    blocks = length // TOK_DEV
    query_blocks = query_nope.reshape(blocks, TOK_DEV, HEADS, NOPE_DIM)
    rope_blocks = query_rope.reshape(blocks, TOK_DEV, HEADS, ROPE_DIM)
    result = lax.map(one_block, (query_blocks, rope_blocks))
    return result.reshape(length, HEADS * VALUE_DIM)

def pooled_mix(pool_in, w_pool_mix):
    length = pool_in.shape[0]
    sums = jnp.pad(jnp.cumsum(pool_in.astype(jnp.float32), axis=0), ((1, 0), (0, 0)))
    position = jnp.arange(length, dtype=jnp.int32)
    outputs = []
    for group, window in enumerate(window_sizes):
        low_edge = jnp.clip(position - window // 2, 0, length)
        high_edge = jnp.clip(position + window - window // 2, 0, length)
        group_sums = sums[:, group * POOL_GROUP:(group + 1) * POOL_GROUP]
        window_mean = (group_sums[high_edge] - group_sums[low_edge]) / (high_edge - low_edge).astype(jnp.float32)[:, None]
        spread = window_mean.astype(jnp.bfloat16) - pool_in[:, group * POOL_GROUP:(group + 1) * POOL_GROUP]
        outputs.append(jnp.dot(spread, w_pool_mix[group], preferred_element_type=jnp.float32).astype(jnp.bfloat16))
    return jnp.concatenate(outputs, axis=1)

def reference(tokens, norm_gain, w_q_down, q_gain, w_q_nope, w_q_rope, w_kv_down, kv_gain, w_k_up, w_v_up, w_k_rope, w_pool_in, w_pool_mix, w_out_attn, w_out_pool):

    def one_sequence(token_rows):
        length = token_rows.shape[0]
        position = jnp.arange(length, dtype=jnp.int32)
        angle_table = angles(position)
        hidden = normed(token_rows, norm_gain)
        q_latent = normed(jnp.dot(hidden, w_q_down, preferred_element_type=jnp.float32).astype(jnp.bfloat16), q_gain)
        kv_latent = normed(jnp.dot(hidden, w_kv_down, preferred_element_type=jnp.float32).astype(jnp.bfloat16), kv_gain)
        query_nope = jnp.dot(q_latent, w_q_nope, preferred_element_type=jnp.float32).astype(jnp.bfloat16)
        query_nope = query_nope.reshape(length, HEADS, NOPE_DIM)
        query_pre = jnp.dot(q_latent, w_q_rope, preferred_element_type=jnp.float32).astype(jnp.bfloat16)
        query_rope = rotate(query_pre.reshape(length, HEADS, ROPE_DIM), angle_table[:, None])
        key_nope = jnp.dot(kv_latent, w_k_up, preferred_element_type=jnp.float32).astype(jnp.bfloat16)
        key_nope = key_nope.reshape(length, HEADS, NOPE_DIM)
        values_all = jnp.dot(kv_latent, w_v_up, preferred_element_type=jnp.float32).astype(jnp.bfloat16)
        values_all = values_all.reshape(length, HEADS, VALUE_DIM)
        key_pre = jnp.dot(hidden, w_k_rope, preferred_element_type=jnp.float32).astype(jnp.bfloat16)
        key_rope = rotate(key_pre, angle_table)
        attended = attend(query_nope, query_rope, key_nope, key_rope, values_all)
        pool_in = jnp.dot(hidden, w_pool_in, preferred_element_type=jnp.float32).astype(jnp.bfloat16)
        pooled = pooled_mix(pool_in, w_pool_mix)
        combined = jnp.dot(attended, w_out_attn, preferred_element_type=jnp.float32)
        combined = combined + jnp.dot(pooled, w_out_pool, preferred_element_type=jnp.float32)
        return combined.astype(jnp.bfloat16)
    return lax.map(one_sequence, tokens)
```

```python
import jax
import jax.numpy as jnp
from jax import lax
from jax.sharding import PartitionSpec as P

NOPE_DIM = 128
ROPE_DIM = 64
VALUE_DIM = 128
GRID_W = 64
POOL_GROUP = 256


EPS = 1e-06
THETA = 10000.0
window_sizes = (2, 4, 8, 16)
rim_width = 8
span_limit = 1024


def padded_2(array, sides, width):
    for axis, dim in sides:
        size, length = (lax.axis_size(axis), array.shape[dim])
        up = [(i, (i + 1) % size) for i in range(size - 1)]
        down = [(j, i) for i, j in up]
        last = lax.slice_in_dim(array, length - width, length, axis=dim)
        first = lax.slice_in_dim(array, 0, width, axis=dim)
        before = lax.ppermute(last, axis, up)
        after = lax.ppermute(first, axis, down)
        array = jnp.concatenate([before, array, after], axis=dim)
    return array


def normed(values, gain_vec):
    widened = values.astype(jnp.float32)
    scaled = widened * lax.rsqrt(jnp.mean(widened * widened, axis=-1, keepdims=True) + EPS)
    return (scaled * gain_vec.astype(jnp.float32)).astype(jnp.bfloat16)


def angles(position):
    row_index = (position // GRID_W).astype(jnp.float32)
    column = (position % GRID_W).astype(jnp.float32)
    inverse = THETA ** (-jnp.arange(0, ROPE_DIM // 2, 2).astype(jnp.float32) / (ROPE_DIM // 2))
    return jnp.stack([row_index, column], axis=-1)[:, :, None] * inverse


def rotate(values, angle_table):
    full_shape = values.shape
    split_parts = values.astype(jnp.float32).reshape(full_shape[:-1] + (2, 2, ROPE_DIM // 4))
    front_half = split_parts[..., 0, :]
    back_half = split_parts[..., 1, :]
    cosine = jnp.cos(angle_table)
    sine_part = jnp.sin(angle_table)
    turned = jnp.stack(
        [front_half * cosine - back_half * sine_part, front_half * sine_part + back_half * cosine],
        axis=-2,
    )
    return turned.reshape(full_shape).astype(jnp.bfloat16)


def swap_tp(array):
    return lax.ppermute(array, "tp", [(0, 1), (1, 0)])


def in_core_order(mine, other, core, axis):
    return jnp.where(
        core == 0,
        jnp.concatenate([mine, other], axis=axis),
        jnp.concatenate([other, mine], axis=axis),
    )


def flip_fs(array, bits):
    size = lax.axis_size("fs")
    return lax.ppermute(array, "fs", [(i, i ^ bits) for i in range(size)])


def row_parts(shard, core):
    rows = shard.shape[0] // 2
    mine = lax.dynamic_slice_in_dim(shard, core * rows, rows, 0)
    by_one = flip_fs(mine, 1)
    by_two = flip_fs(mine, 2)
    far_low = flip_fs(by_two[: rows // 2], 1)
    far_high = flip_fs(by_one[rows // 2 :], 2)
    return mine, by_one, by_two, far_low, far_high


def split_dot(hidden, parts, core):
    mine, by_one, by_two, far_low, far_high = parts
    rows = mine.shape[0]
    here = lax.axis_index("fs")

    def columns(bits, start, count):
        at = (here ^ bits) * (2 * rows) + core * rows + start
        return lax.dynamic_slice_in_dim(hidden, at, count, 1)

    pairs = (
        (columns(0, 0, rows), mine),
        (columns(1, 0, rows), by_one),
        (columns(2, 0, rows), by_two),
        (columns(3, 0, rows // 2), far_low),
        (columns(3, rows // 2, rows // 2), far_high),
    )
    total = 0.0
    for left, right in pairs:
        total = total + jnp.dot(left, right, preferred_element_type=jnp.float32)
    return total + swap_tp(total)


def gather_sp(array):
    size = lax.axis_size("sp")
    if size > 4:
        return lax.all_gather(array, "sp", axis=0, tiled=True)
    here = lax.axis_index("sp")
    rows = array.shape[0]
    out = jnp.zeros((size * rows,) + array.shape[1:], array.dtype)
    out = lax.dynamic_update_slice_in_dim(out, array, here * rows, 0)
    for shift in range(1, size):
        got = lax.ppermute(array, "sp", [(i, (i + shift) % size) for i in range(size)])
        out = lax.dynamic_update_slice_in_dim(out, got, ((here - shift) % size) * rows, 0)
    return out


def key_spans(state_now, members, absorb_span):
    row_count = members[0].shape[0]
    span_rows = 1
    for candidate in range(1, min(row_count, span_limit) + 1):
        if row_count % candidate == 0:
            span_rows = candidate
    if span_rows == row_count:
        return absorb_span(state_now, members)
    stacked = tuple(
        (
            member.reshape((row_count // span_rows, span_rows) + member.shape[1:])
            for member in members
        )
    )

    def advance(carry, member_set):
        return (absorb_span(carry, member_set), None)

    final_state, unused = lax.scan(advance, state_now, stacked)
    return final_state


def on_device(
    tokens,
    norm_gain,
    w_q_down,
    q_gain,
    w_q_nope,
    w_q_rope,
    w_kv_down,
    kv_gain,
    w_k_up,
    w_v_up,
    w_k_rope,
    w_pool_in,
    w_pool_mix,
    w_out_attn,
    w_out_pool,
):
    other_rows, other_gain = swap_tp(tokens[0]), swap_tp(norm_gain)
    core = lax.axis_index("tp")
    token_rows = in_core_order(tokens[0], other_rows, core, 1)
    gathered_gain = in_core_order(norm_gain, other_gain, core, 0)
    local_rows = token_rows.shape[0]
    kv_parts = row_parts(w_kv_down, core)
    q_parts = row_parts(w_q_down, core)
    heads_dev = w_q_nope.shape[1] // NOPE_DIM
    length = local_rows * lax.axis_size("sp")
    position = lax.axis_index("sp") * local_rows + jnp.arange(local_rows, dtype=jnp.int32)
    angle_table = angles(position)
    hidden = normed(token_rows, gathered_gain)
    kv_latent = normed(split_dot(hidden, kv_parts, core).astype(jnp.bfloat16), kv_gain)
    q_latent = normed(split_dot(hidden, q_parts, core).astype(jnp.bfloat16), q_gain)
    query_nope = jnp.dot(q_latent, w_q_nope, preferred_element_type=jnp.float32).astype(
        jnp.bfloat16
    )
    query_nope = query_nope.reshape(local_rows, heads_dev, NOPE_DIM)
    query_pre = jnp.dot(q_latent, w_q_rope, preferred_element_type=jnp.float32).astype(jnp.bfloat16)
    query_rope = rotate(query_pre.reshape(local_rows, heads_dev, ROPE_DIM), angle_table[:, None])
    key_pre = jnp.dot(hidden, w_k_rope, preferred_element_type=jnp.float32).astype(jnp.bfloat16)
    key_rope = rotate(key_pre, angle_table)
    score_scale = (NOPE_DIM + ROPE_DIM) ** (-0.5)

    def absorb(state_now, key_nope, rope_member, values_all):
        running_max, row_total, weighted = state_now
        key_heads = key_nope.reshape(key_nope.shape[0], heads_dev, NOPE_DIM)
        value_heads = values_all.reshape(values_all.shape[0], heads_dev, VALUE_DIM)
        scores = jnp.einsum(
            "qhd,khd->hqk", query_nope, key_heads, preferred_element_type=jnp.float32
        )
        scores = scores + jnp.einsum(
            "qhr,kr->hqk", query_rope, rope_member, preferred_element_type=jnp.float32
        )
        scores = scores * score_scale
        new_max = jnp.maximum(running_max, jnp.max(scores, axis=-1))
        shrink = jnp.exp(running_max - new_max)
        weights = jnp.exp(scores - new_max[:, :, None])
        row_total = row_total * shrink + jnp.sum(weights, axis=-1)
        weighted = weighted * jnp.transpose(shrink)[:, :, None] + jnp.einsum(
            "hqk,khd->qhd",
            weights.astype(jnp.bfloat16),
            value_heads,
            preferred_element_type=jnp.float32,
        )
        return (new_max, row_total, weighted)

    start_state = (
        jnp.full((heads_dev, local_rows), -1e30, jnp.float32),
        jnp.zeros((heads_dev, local_rows), jnp.float32),
        jnp.zeros((local_rows, heads_dev, VALUE_DIM), jnp.float32),
    )

    def latent_span(state_now, members):
        latent_member, rope_member = members
        key_nope = jnp.dot(latent_member, w_k_up, preferred_element_type=jnp.float32).astype(
            jnp.bfloat16
        )
        values_all = jnp.dot(latent_member, w_v_up, preferred_element_type=jnp.float32).astype(
            jnp.bfloat16
        )
        return absorb(state_now, key_nope, rope_member, values_all)

    shared = gather_sp(jnp.concatenate([kv_latent, key_rope], axis=1))
    final_max, row_total, weighted = key_spans(
        start_state,
        (shared[:, : kv_latent.shape[1]], shared[:, kv_latent.shape[1] :]),
        latent_span,
    )
    attended = (weighted / jnp.transpose(row_total)[:, :, None]).astype(jnp.bfloat16)
    attended = attended.reshape(local_rows, heads_dev * VALUE_DIM)
    pool_in = jnp.dot(hidden, w_pool_in, preferred_element_type=jnp.float32).astype(jnp.bfloat16)
    groups_dev = pool_in.shape[1] // POOL_GROUP
    group_id = lax.axis_index("tp") * groups_dev + jnp.arange(groups_dev, dtype=jnp.int32)
    window = jnp.zeros((groups_dev,), jnp.int32)
    for group_index, window_size in enumerate(window_sizes):
        window = window + jnp.where(group_id == group_index, window_size, 0).astype(jnp.int32)
    window = jnp.repeat(window, POOL_GROUP)
    before = window // 2
    window_after = window - before
    padded = padded_2(pool_in, (("sp", 0),), 8)
    padded_wide = padded.astype(jnp.float32)
    window_sum = jnp.zeros(pool_in.shape, jnp.float32)
    for offset in range(-rim_width, rim_width):
        inside = ((offset >= -before) & (offset < window_after)).astype(jnp.float32)
        window_sum = (
            window_sum + padded_wide[rim_width + offset : rim_width + offset + local_rows] * inside
        )
    low_edge = jnp.clip(position[:, None] - before[None, :], 0, length)
    high_edge = jnp.clip(position[:, None] + window_after[None, :], 0, length)
    window_mean = (window_sum / (high_edge - low_edge).astype(jnp.float32)).astype(jnp.bfloat16)
    spread = (window_mean - pool_in).reshape(local_rows, groups_dev, POOL_GROUP)
    mixing = lax.dynamic_slice_in_dim(w_pool_mix, lax.axis_index("tp") * groups_dev, groups_dev, 0)
    pooled = jnp.einsum("tgc,gce->tge", spread, mixing, preferred_element_type=jnp.float32).astype(
        jnp.bfloat16
    )
    pooled = pooled.reshape(local_rows, groups_dev * POOL_GROUP)
    out_partial = jnp.dot(attended, w_out_attn, preferred_element_type=jnp.float32) + jnp.dot(
        pooled, w_out_pool, preferred_element_type=jnp.float32
    )
    half = local_rows // lax.axis_size("tp")
    outgoing = lax.dynamic_slice_in_dim(out_partial, (1 - core) * half, half, 0)
    kept = lax.dynamic_slice_in_dim(out_partial, core * half, half, 0)
    incoming = swap_tp(outgoing.astype(jnp.bfloat16))
    out_share = (kept + incoming.astype(jnp.float32)).astype(jnp.bfloat16)
    return out_share[None]


def solution(mesh):
    placed = (
        P("fs", "sp", "tp"),
        P("tp"),
        P("fs", None),
        P(),
        P(None, "tp"),
        P(None, "tp"),
        P("fs", None),
        P(),
        P(None, "tp"),
        P(None, "tp"),
        P(),
        P(None, "tp"),
        P(),
        P("tp", None),
        P("tp", None),
    )
    return jax.shard_map(
        on_device,
        mesh=mesh,
        in_specs=placed,
        out_specs=P("fs", ("sp", "tp"), None),
        check_vma=False,
    )
```

```python
import jax
import jax.numpy as jnp
from jax import lax
from jax.experimental import pallas as pl
from jax.experimental.pallas import tpu as pltpu
from jax.sharding import PartitionSpec as P

NOPE_DIM = 128
ROPE_DIM = 64
VALUE_DIM = 128
GRID_W = 64
POOL_GROUP = 256


EPS = 1e-06
THETA = 10000.0
window_sizes = (2, 4, 8, 16)
rim_width = 8


def padded_2(array, sides, width):
    for axis, dim in sides:
        size, length = (lax.axis_size(axis), array.shape[dim])
        up = [(i, (i + 1) % size) for i in range(size - 1)]
        down = [(j, i) for i, j in up]
        last = lax.slice_in_dim(array, length - width, length, axis=dim)
        first = lax.slice_in_dim(array, 0, width, axis=dim)
        before = lax.ppermute(last, axis, up)
        after = lax.ppermute(first, axis, down)
        array = jnp.concatenate([before, array, after], axis=dim)
    return array


def position_tables(position, lanes):
    lane = jnp.arange(lanes, dtype=jnp.int32)
    row_index = (position // GRID_W).astype(jnp.float32)[:, None]
    column = (position % GRID_W).astype(jnp.float32)[:, None]
    quarter = ROPE_DIM // 4
    in_row = (lane % ROPE_DIM) < 2 * quarter
    step = (2 * (lane % quarter)).astype(jnp.float32)
    inverse = THETA ** (-step / (ROPE_DIM // 2))
    angle = jnp.where(in_row[None, :], row_index, column) * inverse[None, :]
    return jnp.cos(angle), jnp.sin(angle)


def turning_matrix(lanes):
    quarter = ROPE_DIM // 4
    source = lax.broadcasted_iota(jnp.int32, (lanes, lanes), 0)
    target = lax.broadcasted_iota(jnp.int32, (lanes, lanes), 1)
    first = (target % (2 * quarter)) < quarter
    minus = jnp.where(first & (source == target + quarter), -1.0, 0.0)
    plus = jnp.where((~first) & (source == target - quarter), 1.0, 0.0)
    return (minus + plus).astype(jnp.bfloat16)


def turned(values, cosine, sine):
    swapped = jnp.dot(
        values, turning_matrix(values.shape[1]), preferred_element_type=jnp.float32
    )
    return (values.astype(jnp.float32) * cosine + swapped * sine).astype(jnp.bfloat16)


def normed(values, gain_vec):
    widened = values.astype(jnp.float32)
    scaled = widened * lax.rsqrt(jnp.mean(widened * widened, axis=-1, keepdims=True) + EPS)
    return (scaled * gain_vec.astype(jnp.float32)).astype(jnp.bfloat16)


def front_kernel(
    core, mine, other, gain_mine, gain_other, w_pool, w_key, cosine, sine, hidden, pool_in, key_rope
):
    width = mine.shape[1]
    left = mine[...].astype(jnp.float32)
    right = other[...].astype(jnp.float32)
    squares = jnp.sum(left * left, axis=1, keepdims=True)
    squares = squares + jnp.sum(right * right, axis=1, keepdims=True)
    factor = lax.rsqrt(squares / (2 * width) + EPS)
    here = pl.multiple_of(core[0] * width, width)
    there = pl.multiple_of((1 - core[0]) * width, width)
    hidden[:, pl.ds(here, width)] = (left * factor * gain_mine[...].astype(jnp.float32)).astype(
        jnp.bfloat16
    )
    hidden[:, pl.ds(there, width)] = (right * factor * gain_other[...].astype(jnp.float32)).astype(
        jnp.bfloat16
    )
    rows = hidden[...]
    key_pre = jnp.dot(rows, w_key[...], preferred_element_type=jnp.float32).astype(jnp.bfloat16)
    key_rope[...] = turned(key_pre, cosine[:, :ROPE_DIM], sine[:, :ROPE_DIM])
    pool_in[...] = jnp.dot(rows, w_pool[...], preferred_element_type=jnp.float32).astype(
        jnp.bfloat16
    )


def part_kernel(starts, hidden, *refs):
    parts, out = refs[:-1], refs[-1]
    total = None
    for index, part in enumerate(parts):
        rows = part.shape[0]
        left = hidden[:, pl.ds(pl.multiple_of(starts[index], rows), rows)]
        share = jnp.dot(left, part[...], preferred_element_type=jnp.float32)
        total = share if total is None else total + share
    out[...] = total


def latent_kernel(mine, other, gain, key_rope, out):
    summed = (mine[...] + other[...]).astype(jnp.bfloat16)
    rank = summed.shape[1]
    out[:, :rank] = normed(summed, gain[...])
    out[:, rank:] = key_rope[...]


def attend_kernel(count):
    def body(core, q_mine, q_other, q_gain, cosine, sine, pooled, *refs):
        pieces = refs[:count]
        w_qn, w_qr, w_k, w_v, w_attn, w_pool, kept, outgoing = refs[count : count + 8]
        q_latent, latent, rope_twice, total = refs[count + 8 :]
        step = pl.program_id(0)
        rank = latent.shape[1]

        @pl.when(step == 0)
        def _():
            q_latent[...] = normed((q_mine[...] + q_other[...]).astype(jnp.bfloat16), q_gain[...])
            source = lax.broadcasted_iota(jnp.int32, (ROPE_DIM, 2 * ROPE_DIM), 0)
            target = lax.broadcasted_iota(jnp.int32, (ROPE_DIM, 2 * ROPE_DIM), 1)
            twice = jnp.where(target % ROPE_DIM == source, 1.0, 0.0).astype(jnp.bfloat16)
            at = 0
            for piece in pieces:
                rows = piece.shape[0]
                latent[at : at + rows, :] = piece[:, :rank]
                rope_twice[at : at + rows, :] = jnp.dot(
                    piece[:, rank:], twice, preferred_element_type=jnp.float32
                ).astype(jnp.bfloat16)
                at += rows
            total[...] = jnp.zeros(total.shape, jnp.float32)

        q_rows = q_latent[...]
        query = jnp.dot(q_rows, w_qn[...], preferred_element_type=jnp.float32).astype(jnp.bfloat16)
        pre = jnp.dot(q_rows, w_qr[...], preferred_element_type=jnp.float32).astype(jnp.bfloat16)
        rope = turned(pre, cosine[...], sine[...])
        keys = jnp.dot(latent[...], w_k[...], preferred_element_type=jnp.float32).astype(
            jnp.bfloat16
        )
        values = jnp.dot(latent[...], w_v[...], preferred_element_type=jnp.float32).astype(
            jnp.bfloat16
        )
        lane = lax.broadcasted_iota(jnp.int32, rope.shape, 1)
        factor = (NOPE_DIM + ROPE_DIM) ** (-0.5) * 1.4426950408889634
        features = []
        for head in range(2):
            own = (lane // ROPE_DIM) == head
            rope_head = jnp.where(own, rope.astype(jnp.float32), 0.0).astype(jnp.bfloat16)
            left = jnp.concatenate(
                [query[:, head * NOPE_DIM : (head + 1) * NOPE_DIM], rope_head], axis=1
            )
            right = jnp.concatenate(
                [keys[:, head * NOPE_DIM : (head + 1) * NOPE_DIM], rope_twice[...]], axis=1
            )
            scores = lax.dot_general(
                left, right, (((1,), (1,)), ((), ())), preferred_element_type=jnp.float32
            )
            top = jnp.max(scores, axis=1, keepdims=True)
            weights = jnp.exp2((scores - top) * factor)
            row_total = jnp.sum(weights, axis=1, keepdims=True)
            summed = jnp.dot(
                weights.astype(jnp.bfloat16),
                values[:, head * VALUE_DIM : (head + 1) * VALUE_DIM],
                preferred_element_type=jnp.float32,
            )
            features.append((summed / row_total).astype(jnp.bfloat16))
        attended = jnp.concatenate(features, axis=1)
        total[...] += jnp.dot(
            attended, w_attn[...], preferred_element_type=jnp.float32
        ) + jnp.dot(pooled[...], w_pool[...], preferred_element_type=jnp.float32)

        @pl.when(step == pl.num_programs(0) - 1)
        def _():
            half = kept.shape[0]
            kept[...] = total[pl.ds(pl.multiple_of(core[0] * half, 8), half), :]
            outgoing[...] = total[pl.ds(pl.multiple_of((1 - core[0]) * half, 8), half), :].astype(
                jnp.bfloat16
            )

    return body


def whole_call(kernel, shapes, scalars, *arrays):
    return pl.pallas_call(
        kernel,
        out_shape=shapes,
        in_specs=[pl.BlockSpec(memory_space=pltpu.SMEM)] * len(scalars)
        + [pl.BlockSpec(memory_space=pltpu.VMEM)] * len(arrays),
        out_specs=jax.tree.map(lambda _: pl.BlockSpec(memory_space=pltpu.VMEM), shapes),
    )(*scalars, *arrays)


def swap_tp(array):
    return lax.ppermute(array, "tp", [(0, 1), (1, 0)])


def flip_fs(array, bits):
    size = lax.axis_size("fs")
    return lax.ppermute(array, "fs", [(i, i ^ bits) for i in range(size)])


def row_parts(shard, core):
    rows = shard.shape[0] // 2
    mine = lax.dynamic_slice_in_dim(shard, core * rows, rows, 0)
    return (mine,) + tuple((flip_fs(mine, bits) for bits in range(1, lax.axis_size("fs"))))


def split_dot(hidden, parts, core):
    rows = parts[0].shape[0]
    here = lax.axis_index("fs")
    starts = (here ^ jnp.arange(len(parts), dtype=jnp.int32)) * (2 * rows) + core * rows
    shape = jax.ShapeDtypeStruct((hidden.shape[0], parts[0].shape[1]), jnp.float32)
    return whole_call(part_kernel, shape, (starts,), hidden, *parts)


def gather_sp(array):
    size = lax.axis_size("sp")
    if size > 4:
        return (lax.all_gather(array, "sp", axis=0, tiled=True),)
    pieces = [array]
    for shift in range(1, size):
        pieces.append(lax.ppermute(array, "sp", [(i, (i + shift) % size) for i in range(size)]))
    return tuple(pieces)


def on_device(
    tokens,
    norm_gain,
    w_q_down,
    q_gain,
    w_q_nope,
    w_q_rope,
    w_kv_down,
    kv_gain,
    w_k_up,
    w_v_up,
    w_k_rope,
    w_pool_in,
    w_pool_mix,
    w_out_attn,
    w_out_pool,
):
    core = lax.axis_index("tp")
    core_ref = core.astype(jnp.int32).reshape(1)
    own_rows = tokens[0]
    other_rows, other_gain = swap_tp(own_rows), swap_tp(norm_gain)
    kv_parts = row_parts(w_kv_down, core)
    q_parts = row_parts(w_q_down, core)
    local_rows = own_rows.shape[0]
    length = local_rows * lax.axis_size("sp")
    position = lax.axis_index("sp") * local_rows + jnp.arange(local_rows, dtype=jnp.int32)
    cosine, sine = position_tables(position, 2 * ROPE_DIM)
    width = 2 * own_rows.shape[1]
    hidden, pool_in, key_rope = whole_call(
        front_kernel,
        (
            jax.ShapeDtypeStruct((local_rows, width), jnp.bfloat16),
            jax.ShapeDtypeStruct((local_rows, w_pool_in.shape[1]), jnp.bfloat16),
            jax.ShapeDtypeStruct((local_rows, ROPE_DIM), jnp.bfloat16),
        ),
        (core_ref,),
        own_rows,
        other_rows,
        norm_gain[None],
        other_gain[None],
        w_pool_in,
        w_k_rope,
        cosine,
        sine,
    )
    kv_share = split_dot(hidden, kv_parts, core)
    kv_rank = kv_share.shape[1]
    shared = whole_call(
        latent_kernel,
        jax.ShapeDtypeStruct((local_rows, kv_rank + ROPE_DIM), jnp.bfloat16),
        (),
        kv_share,
        swap_tp(kv_share),
        kv_gain[None],
        key_rope,
    )
    pieces = gather_sp(shared)
    q_share = split_dot(hidden, q_parts, core)
    q_other = swap_tp(q_share)
    groups_dev = pool_in.shape[1] // POOL_GROUP
    group_id = lax.axis_index("tp") * groups_dev + jnp.arange(groups_dev, dtype=jnp.int32)
    window = jnp.zeros((groups_dev,), jnp.int32)
    for group_index, window_size in enumerate(window_sizes):
        window = window + jnp.where(group_id == group_index, window_size, 0).astype(jnp.int32)
    window = jnp.repeat(window, POOL_GROUP)
    before = window // 2
    window_after = window - before
    padded = padded_2(pool_in, (("sp", 0),), 8)
    padded_wide = padded.astype(jnp.float32)
    window_sum = jnp.zeros(pool_in.shape, jnp.float32)
    for offset in range(-rim_width, rim_width):
        inside = ((offset >= -before) & (offset < window_after)).astype(jnp.float32)
        window_sum = (
            window_sum + padded_wide[rim_width + offset : rim_width + offset + local_rows] * inside
        )
    low_edge = jnp.clip(position[:, None] - before[None, :], 0, length)
    high_edge = jnp.clip(position[:, None] + window_after[None, :], 0, length)
    window_mean = (window_sum / (high_edge - low_edge).astype(jnp.float32)).astype(jnp.bfloat16)
    spread = (window_mean - pool_in).reshape(local_rows, groups_dev, POOL_GROUP)
    mixing = lax.dynamic_slice_in_dim(w_pool_mix, lax.axis_index("tp") * groups_dev, groups_dev, 0)
    pooled = jnp.einsum("tgc,gce->tge", spread, mixing, preferred_element_type=jnp.float32).astype(
        jnp.bfloat16
    )
    pooled = pooled.reshape(local_rows, groups_dev * POOL_GROUP)
    steps = w_q_nope.shape[1] // (2 * NOPE_DIM)
    q_rank, features = q_share.shape[1], w_out_attn.shape[1]
    half = local_rows // 2
    pool_rows = pooled.shape[1] // steps

    def fixed(array):
        return pl.BlockSpec(array.shape, lambda p: (0, 0))

    def by_column(array):
        return pl.BlockSpec((array.shape[0], array.shape[1] // steps), lambda p: (0, p))

    def by_row(array):
        return pl.BlockSpec((array.shape[0] // steps, array.shape[1]), lambda p: (p, 0))

    kept, outgoing = pl.pallas_call(
        attend_kernel(len(pieces)),
        grid=(steps,),
        in_specs=[
            pl.BlockSpec(memory_space=pltpu.SMEM),
            fixed(q_share),
            fixed(q_other),
            fixed(q_gain[None]),
            fixed(cosine),
            fixed(sine),
            by_column(pooled),
        ]
        + [fixed(piece) for piece in pieces]
        + [by_column(w) for w in (w_q_nope, w_q_rope, w_k_up, w_v_up)]
        + [by_row(w_out_attn), by_row(w_out_pool)],
        out_specs=(
            pl.BlockSpec((half, features), lambda p: (0, 0)),
            pl.BlockSpec((half, features), lambda p: (0, 0)),
        ),
        out_shape=(
            jax.ShapeDtypeStruct((half, features), jnp.float32),
            jax.ShapeDtypeStruct((half, features), jnp.bfloat16),
        ),
        scratch_shapes=[
            pltpu.VMEM((local_rows, q_rank), jnp.bfloat16),
            pltpu.VMEM((length, kv_rank), jnp.bfloat16),
            pltpu.VMEM((length, 2 * ROPE_DIM), jnp.bfloat16),
            pltpu.VMEM((local_rows, features), jnp.float32),
        ],
        compiler_params=pltpu.CompilerParams(dimension_semantics=("arbitrary",)),
    )(
        core_ref,
        q_share,
        q_other,
        q_gain[None],
        cosine,
        sine,
        pooled,
        *pieces,
        w_q_nope,
        w_q_rope,
        w_k_up,
        w_v_up,
        w_out_attn,
        w_out_pool,
    )
    incoming = swap_tp(outgoing)
    out_share = (kept + incoming.astype(jnp.float32)).astype(jnp.bfloat16)
    return out_share[None]


def solution(mesh):
    placed = (
        P("fs", "sp", "tp"),
        P("tp"),
        P("fs", None),
        P(),
        P(None, "tp"),
        P(None, "tp"),
        P("fs", None),
        P(),
        P(None, "tp"),
        P(None, "tp"),
        P(),
        P(None, "tp"),
        P(),
        P("tp", None),
        P("tp", None),
    )
    return jax.shard_map(
        on_device,
        mesh=mesh,
        in_specs=placed,
        out_specs=P("fs", ("sp", "tp"), None),
        check_vma=False,
    )
```

```python
import jax
import jax.numpy as jnp
from jax import lax
from jax.experimental import pallas as pl
from jax.experimental.pallas import tpu as pltpu
from jax.sharding import PartitionSpec as P

NOPE_DIM = 128
ROPE_DIM = 64
VALUE_DIM = 128
GRID_W = 64
POOL_GROUP = 256


EPS = 1e-06
THETA = 10000.0
window_sizes = (2, 4, 8, 16)
rim_width = 8


def padded_2(array, sides, width):
    for axis, dim in sides:
        size, length = (lax.axis_size(axis), array.shape[dim])
        up = [(i, (i + 1) % size) for i in range(size - 1)]
        down = [(j, i) for i, j in up]
        last = lax.slice_in_dim(array, length - width, length, axis=dim)
        first = lax.slice_in_dim(array, 0, width, axis=dim)
        before = lax.ppermute(last, axis, up)
        after = lax.ppermute(first, axis, down)
        array = jnp.concatenate([before, array, after], axis=dim)
    return array


def position_tables(position, lanes):
    lane = jnp.arange(lanes, dtype=jnp.int32)
    row_index = (position // GRID_W).astype(jnp.float32)[:, None]
    column = (position % GRID_W).astype(jnp.float32)[:, None]
    quarter = ROPE_DIM // 4
    in_row = (lane % ROPE_DIM) < 2 * quarter
    step = (2 * (lane % quarter)).astype(jnp.float32)
    inverse = THETA ** (-step / (ROPE_DIM // 2))
    angle = jnp.where(in_row[None, :], row_index, column) * inverse[None, :]
    return jnp.cos(angle), jnp.sin(angle)


def turning_matrix(lanes):
    quarter = ROPE_DIM // 4
    source = lax.broadcasted_iota(jnp.int32, (lanes, lanes), 0)
    target = lax.broadcasted_iota(jnp.int32, (lanes, lanes), 1)
    first = (target % (2 * quarter)) < quarter
    minus = jnp.where(first & (source == target + quarter), -1.0, 0.0)
    plus = jnp.where((~first) & (source == target - quarter), 1.0, 0.0)
    return (minus + plus).astype(jnp.bfloat16)


def turned(values, cosine, sine):
    swapped = jnp.dot(
        values, turning_matrix(values.shape[1]), preferred_element_type=jnp.float32
    )
    return (values.astype(jnp.float32) * cosine + swapped * sine).astype(jnp.bfloat16)


def normed(values, gain_vec):
    widened = values.astype(jnp.float32)
    scaled = widened * lax.rsqrt(jnp.mean(widened * widened, axis=-1, keepdims=True) + EPS)
    return (scaled * gain_vec.astype(jnp.float32)).astype(jnp.bfloat16)


def front_kernel(
    core, mine, other, gain_mine, gain_other, w_pool, w_key, cosine, sine, hidden, pool_in, key_rope
):
    width = mine.shape[1]
    left = mine[...].astype(jnp.float32)
    right = other[...].astype(jnp.float32)
    squares = jnp.sum(left * left, axis=1, keepdims=True)
    squares = squares + jnp.sum(right * right, axis=1, keepdims=True)
    factor = lax.rsqrt(squares / (2 * width) + EPS)
    here = pl.multiple_of(core[0] * width, width)
    there = pl.multiple_of((1 - core[0]) * width, width)
    hidden[:, pl.ds(here, width)] = (left * factor * gain_mine[...].astype(jnp.float32)[None, :]).astype(
        jnp.bfloat16
    )
    hidden[:, pl.ds(there, width)] = (right * factor * gain_other[...].astype(jnp.float32)[None, :]).astype(
        jnp.bfloat16
    )
    rows = hidden[...]
    key_pre = lax.dot_general(
        rows, w_key[...], (((1,), (1,)), ((), ())), preferred_element_type=jnp.float32
    ).astype(jnp.bfloat16)
    key_rope[...] = turned(key_pre, cosine[:, :ROPE_DIM], sine[:, :ROPE_DIM])
    pool_in[...] = jnp.dot(rows, w_pool[...], preferred_element_type=jnp.float32).astype(
        jnp.bfloat16
    )


def part_kernel(starts, hidden, *refs):
    parts, out = refs[:-1], refs[-1]
    total = None
    for index, part in enumerate(parts):
        rows = part.shape[0]
        left = hidden[:, pl.ds(pl.multiple_of(starts[index], rows), rows)]
        share = jnp.dot(left, part[...], preferred_element_type=jnp.float32)
        total = share if total is None else total + share
    out[...] = total


def latent_kernel(mine, other, gain, key_rope, out):
    summed = (mine[...] + other[...]).astype(jnp.bfloat16)
    rank = summed.shape[1]
    out[:, :rank] = normed(summed, gain[...])
    out[:, rank:] = key_rope[...]


def attend_kernel(count):
    def body(core, q_mine, q_other, q_gain, cosine, sine, pooled, *refs):
        pieces = refs[:count]
        w_qn, w_qr, w_k, w_v, w_attn, w_pool, kept, outgoing = refs[count : count + 8]
        q_latent, latent, rope_twice, total = refs[count + 8 :]
        step = pl.program_id(0)
        rank = latent.shape[1]

        @pl.when(step == 0)
        def _():
            q_latent[...] = normed((q_mine[...] + q_other[...]).astype(jnp.bfloat16), q_gain[...])
            source = lax.broadcasted_iota(jnp.int32, (ROPE_DIM, 2 * ROPE_DIM), 0)
            target = lax.broadcasted_iota(jnp.int32, (ROPE_DIM, 2 * ROPE_DIM), 1)
            twice = jnp.where(target % ROPE_DIM == source, 1.0, 0.0).astype(jnp.bfloat16)
            at = 0
            for piece in pieces:
                rows = piece.shape[0]
                latent[at : at + rows, :] = piece[:, :rank]
                rope_twice[at : at + rows, :] = jnp.dot(
                    piece[:, rank:], twice, preferred_element_type=jnp.float32
                ).astype(jnp.bfloat16)
                at += rows
            total[...] = jnp.zeros(total.shape, jnp.float32)

        q_rows = q_latent[...]
        query = jnp.dot(q_rows, w_qn[...], preferred_element_type=jnp.float32).astype(jnp.bfloat16)
        pre = jnp.dot(q_rows, w_qr[...], preferred_element_type=jnp.float32).astype(jnp.bfloat16)
        rope = turned(pre, cosine[...], sine[...])
        keys = jnp.dot(latent[...], w_k[...], preferred_element_type=jnp.float32).astype(
            jnp.bfloat16
        )
        values = jnp.dot(latent[...], w_v[...], preferred_element_type=jnp.float32).astype(
            jnp.bfloat16
        )
        lane = lax.broadcasted_iota(jnp.int32, rope.shape, 1)
        factor = (NOPE_DIM + ROPE_DIM) ** (-0.5) * 1.4426950408889634
        features = []
        for head in range(2):
            own = (lane // ROPE_DIM) == head
            rope_head = jnp.where(own, rope.astype(jnp.float32), 0.0).astype(jnp.bfloat16)
            left = jnp.concatenate(
                [query[:, head * NOPE_DIM : (head + 1) * NOPE_DIM], rope_head], axis=1
            )
            right = jnp.concatenate(
                [keys[:, head * NOPE_DIM : (head + 1) * NOPE_DIM], rope_twice[...]], axis=1
            )
            scores = lax.dot_general(
                left, right, (((1,), (1,)), ((), ())), preferred_element_type=jnp.float32
            )
            top = jnp.max(scores, axis=1, keepdims=True)
            weights = jnp.exp2((scores - top) * factor)
            row_total = jnp.sum(weights, axis=1, keepdims=True)
            summed = jnp.dot(
                weights.astype(jnp.bfloat16),
                values[:, head * VALUE_DIM : (head + 1) * VALUE_DIM],
                preferred_element_type=jnp.float32,
            )
            features.append((summed / row_total).astype(jnp.bfloat16))
        attended = jnp.concatenate(features, axis=1)
        total[...] += jnp.dot(
            attended, w_attn[...], preferred_element_type=jnp.float32
        ) + jnp.dot(pooled[...], w_pool[...], preferred_element_type=jnp.float32)

        @pl.when(step == pl.num_programs(0) - 1)
        def _():
            half = kept.shape[0]
            kept[...] = total[pl.ds(pl.multiple_of(core[0] * half, 8), half), :]
            outgoing[...] = total[pl.ds(pl.multiple_of((1 - core[0]) * half, 8), half), :].astype(
                jnp.bfloat16
            )

    return body


def whole_call(kernel, shapes, scalars, *arrays):
    return pl.pallas_call(
        kernel,
        out_shape=shapes,
        in_specs=[pl.BlockSpec(memory_space=pltpu.SMEM)] * len(scalars)
        + [pl.BlockSpec(memory_space=pltpu.VMEM)] * len(arrays),
        out_specs=jax.tree.map(lambda _: pl.BlockSpec(memory_space=pltpu.VMEM), shapes),
    )(*scalars, *arrays)


def swap_tp(array):
    return lax.ppermute(array, "tp", [(0, 1), (1, 0)])


def flip_fs(array, bits):
    size = lax.axis_size("fs")
    return lax.ppermute(array, "fs", [(i, i ^ bits) for i in range(size)])


def row_parts(shard, core):
    rows = shard.shape[0] // 2
    mine = lax.dynamic_slice_in_dim(shard, core * rows, rows, 0)
    return (mine,) + tuple((flip_fs(mine, bits) for bits in range(1, lax.axis_size("fs"))))


def split_dot(hidden, parts, core):
    rows = parts[0].shape[0]
    here = lax.axis_index("fs")
    starts = (here ^ jnp.arange(len(parts), dtype=jnp.int32)) * (2 * rows) + core * rows
    shape = jax.ShapeDtypeStruct((hidden.shape[0], parts[0].shape[1]), jnp.float32)
    return whole_call(part_kernel, shape, (starts,), hidden, *parts)


def gather_sp(array):
    size = lax.axis_size("sp")
    if size > 4:
        return (lax.all_gather(array, "sp", axis=0, tiled=True),)
    pieces = [array]
    for shift in range(1, size):
        pieces.append(lax.ppermute(array, "sp", [(i, (i + shift) % size) for i in range(size)]))
    return tuple(pieces)


def on_device(
    tokens,
    norm_gain,
    w_q_down,
    q_gain,
    w_q_nope,
    w_q_rope,
    w_kv_down,
    kv_gain,
    w_k_up,
    w_v_up,
    w_k_rope,
    w_pool_in,
    w_pool_mix,
    w_out_attn,
    w_out_pool,
):
    core = lax.axis_index("tp")
    core_ref = core.astype(jnp.int32).reshape(1)
    own_rows = tokens[0]
    other_rows, other_gain = swap_tp(own_rows), swap_tp(norm_gain)
    kv_parts = row_parts(w_kv_down, core)
    q_parts = row_parts(w_q_down, core)
    local_rows = own_rows.shape[0]
    length = local_rows * lax.axis_size("sp")
    position = lax.axis_index("sp") * local_rows + jnp.arange(local_rows, dtype=jnp.int32)
    cosine, sine = position_tables(position, 2 * ROPE_DIM)
    width = 2 * own_rows.shape[1]
    hidden, pool_in, key_rope = whole_call(
        front_kernel,
        (
            jax.ShapeDtypeStruct((local_rows, width), jnp.bfloat16),
            jax.ShapeDtypeStruct((local_rows, w_pool_in.shape[1]), jnp.bfloat16),
            jax.ShapeDtypeStruct((local_rows, ROPE_DIM), jnp.bfloat16),
        ),
        (core_ref,),
        own_rows,
        other_rows,
        norm_gain,
        other_gain,
        w_pool_in,
        w_k_rope.T,
        cosine,
        sine,
    )
    kv_share = split_dot(hidden, kv_parts, core)
    kv_rank = kv_share.shape[1]
    shared = whole_call(
        latent_kernel,
        jax.ShapeDtypeStruct((local_rows, kv_rank + ROPE_DIM), jnp.bfloat16),
        (),
        kv_share,
        swap_tp(kv_share),
        kv_gain[None],
        key_rope,
    )
    pieces = gather_sp(shared)
    late_hidden, late_pool, _ = lax.optimization_barrier((hidden, pool_in, shared))
    q_share = split_dot(late_hidden, q_parts, core)
    q_other = swap_tp(q_share)
    groups_dev = pool_in.shape[1] // POOL_GROUP
    group_id = lax.axis_index("tp") * groups_dev + jnp.arange(groups_dev, dtype=jnp.int32)
    window = jnp.zeros((groups_dev,), jnp.int32)
    for group_index, window_size in enumerate(window_sizes):
        window = window + jnp.where(group_id == group_index, window_size, 0).astype(jnp.int32)
    window = jnp.repeat(window, POOL_GROUP)
    before = window // 2
    window_after = window - before
    padded = padded_2(late_pool, (("sp", 0),), 8)
    padded_wide = padded.astype(jnp.float32)
    window_sum = jnp.zeros(pool_in.shape, jnp.float32)
    for offset in range(-rim_width, rim_width):
        inside = ((offset >= -before) & (offset < window_after)).astype(jnp.float32)
        window_sum = (
            window_sum + padded_wide[rim_width + offset : rim_width + offset + local_rows] * inside
        )
    low_edge = jnp.clip(position[:, None] - before[None, :], 0, length)
    high_edge = jnp.clip(position[:, None] + window_after[None, :], 0, length)
    window_mean = (window_sum / (high_edge - low_edge).astype(jnp.float32)).astype(jnp.bfloat16)
    spread = (window_mean - pool_in).reshape(local_rows, groups_dev, POOL_GROUP)
    mixing = lax.dynamic_slice_in_dim(w_pool_mix, lax.axis_index("tp") * groups_dev, groups_dev, 0)
    pooled = jnp.einsum("tgc,gce->tge", spread, mixing, preferred_element_type=jnp.float32).astype(
        jnp.bfloat16
    )
    pooled = pooled.reshape(local_rows, groups_dev * POOL_GROUP)
    steps = w_q_nope.shape[1] // (2 * NOPE_DIM)
    q_rank, features = q_share.shape[1], w_out_attn.shape[1]
    half = local_rows // 2
    pool_rows = pooled.shape[1] // steps

    def fixed(array):
        return pl.BlockSpec(array.shape, lambda p: (0, 0))

    def by_column(array):
        return pl.BlockSpec((array.shape[0], array.shape[1] // steps), lambda p: (0, p))

    def by_row(array):
        return pl.BlockSpec((array.shape[0] // steps, array.shape[1]), lambda p: (p, 0))

    kept, outgoing = pl.pallas_call(
        attend_kernel(len(pieces)),
        grid=(steps,),
        in_specs=[
            pl.BlockSpec(memory_space=pltpu.SMEM),
            fixed(q_share),
            fixed(q_other),
            fixed(q_gain[None]),
            fixed(cosine),
            fixed(sine),
            by_column(pooled),
        ]
        + [fixed(piece) for piece in pieces]
        + [by_column(w) for w in (w_q_nope, w_q_rope, w_k_up, w_v_up)]
        + [by_row(w_out_attn), by_row(w_out_pool)],
        out_specs=(
            pl.BlockSpec((half, features), lambda p: (0, 0)),
            pl.BlockSpec((half, features), lambda p: (0, 0)),
        ),
        out_shape=(
            jax.ShapeDtypeStruct((half, features), jnp.float32),
            jax.ShapeDtypeStruct((half, features), jnp.bfloat16),
        ),
        scratch_shapes=[
            pltpu.VMEM((local_rows, q_rank), jnp.bfloat16),
            pltpu.VMEM((length, kv_rank), jnp.bfloat16),
            pltpu.VMEM((length, 2 * ROPE_DIM), jnp.bfloat16),
            pltpu.VMEM((local_rows, features), jnp.float32),
        ],
        compiler_params=pltpu.CompilerParams(dimension_semantics=("arbitrary",)),
    )(
        core_ref,
        q_share,
        q_other,
        q_gain[None],
        cosine,
        sine,
        pooled,
        *pieces,
        w_q_nope,
        w_q_rope,
        w_k_up,
        w_v_up,
        w_out_attn,
        w_out_pool,
    )
    incoming = swap_tp(outgoing)
    out_share = (kept + incoming.astype(jnp.float32)).astype(jnp.bfloat16)
    return out_share[None]


def solution(mesh):
    placed = (
        P("fs", "sp", "tp"),
        P("tp"),
        P("fs", None),
        P(),
        P(None, "tp"),
        P(None, "tp"),
        P("fs", None),
        P(),
        P(None, "tp"),
        P(None, "tp"),
        P(),
        P(None, "tp"),
        P(),
        P("tp", None),
        P("tp", None),
    )
    return jax.shard_map(
        on_device,
        mesh=mesh,
        in_specs=placed,
        out_specs=P("fs", ("sp", "tp"), None),
        check_vma=False,
    )
```

```python
import jax
import jax.numpy as jnp
from jax import lax
from jax.experimental import pallas as pl
from jax.experimental.pallas import tpu as pltpu
from jax.sharding import PartitionSpec as P

NOPE_DIM = 128
ROPE_DIM = 64
VALUE_DIM = 128
GRID_W = 64
POOL_GROUP = 256


EPS = 1e-06
THETA = 10000.0
window_sizes = (2, 4, 8, 16)
rim_width = 8


def position_tables(position, lanes):
    lane = jnp.arange(lanes, dtype=jnp.int32)
    row_index = (position // GRID_W).astype(jnp.float32)[:, None]
    column = (position % GRID_W).astype(jnp.float32)[:, None]
    quarter = ROPE_DIM // 4
    in_row = (lane % ROPE_DIM) < 2 * quarter
    step = (2 * (lane % quarter)).astype(jnp.float32)
    inverse = THETA ** (-step / (ROPE_DIM // 2))
    angle = jnp.where(in_row[None, :], row_index, column) * inverse[None, :]
    return jnp.cos(angle), jnp.sin(angle)


def turning_matrix(lanes):
    quarter = ROPE_DIM // 4
    source = lax.broadcasted_iota(jnp.int32, (lanes, lanes), 0)
    target = lax.broadcasted_iota(jnp.int32, (lanes, lanes), 1)
    first = (target % (2 * quarter)) < quarter
    minus = jnp.where(first & (source == target + quarter), -1.0, 0.0)
    plus = jnp.where((~first) & (source == target - quarter), 1.0, 0.0)
    return (minus + plus).astype(jnp.bfloat16)


def turned(values, cosine, sine):
    swapped = jnp.dot(
        values, turning_matrix(values.shape[1]), preferred_element_type=jnp.float32
    )
    return (values.astype(jnp.float32) * cosine + swapped * sine).astype(jnp.bfloat16)


def normed(values, gain_vec):
    widened = values.astype(jnp.float32)
    scaled = widened * lax.rsqrt(jnp.mean(widened * widened, axis=-1, keepdims=True) + EPS)
    return (scaled * gain_vec.astype(jnp.float32)).astype(jnp.bfloat16)


def front_kernel(
    core, mine, other, gain_mine, gain_other, w_pool, w_key, cosine, sine, hidden, pool_in, key_rope
):
    width = mine.shape[1]
    left = mine[...].astype(jnp.float32)
    right = other[...].astype(jnp.float32)
    squares = jnp.sum(left * left, axis=1, keepdims=True)
    squares = squares + jnp.sum(right * right, axis=1, keepdims=True)
    factor = lax.rsqrt(squares / (2 * width) + EPS)
    here = pl.multiple_of(core[0] * width, width)
    there = pl.multiple_of((1 - core[0]) * width, width)
    hidden[:, pl.ds(here, width)] = (left * factor * gain_mine[...].astype(jnp.float32)[None, :]).astype(
        jnp.bfloat16
    )
    hidden[:, pl.ds(there, width)] = (right * factor * gain_other[...].astype(jnp.float32)[None, :]).astype(
        jnp.bfloat16
    )
    rows = hidden[...]
    key_pre = lax.dot_general(
        rows, w_key[...], (((1,), (1,)), ((), ())), preferred_element_type=jnp.float32
    ).astype(jnp.bfloat16)
    key_rope[...] = turned(key_pre, cosine[:, :ROPE_DIM], sine[:, :ROPE_DIM])
    pool_in[...] = jnp.dot(rows, w_pool[...], preferred_element_type=jnp.float32).astype(
        jnp.bfloat16
    )


def part_kernel(starts, hidden, *refs):
    parts, out = refs[:-1], refs[-1]
    total = None
    for index, part in enumerate(parts):
        rows = part.shape[0]
        left = hidden[:, pl.ds(pl.multiple_of(starts[index], rows), rows)]
        share = jnp.dot(left, part[...], preferred_element_type=jnp.float32)
        total = share if total is None else total + share
    out[...] = total


def latent_kernel(mine, other, gain, key_rope, pool_in, out):
    summed = (mine[...] + other[...]).astype(jnp.bfloat16)
    rank = summed.shape[1]
    rows = summed.shape[0]
    out[:rows, :rank] = normed(summed, gain[...])
    out[:rows, rank:] = key_rope[...]
    tall = 2 * rim_width
    first = pool_in[:tall, :].astype(jnp.float32)[:rim_width]
    last = pool_in[rows - tall :, :].astype(jnp.float32)[rim_width:]
    edge = jnp.concatenate([first, last], axis=0).astype(jnp.bfloat16)
    for index in range(edge.shape[1] // rank):
        at = rows + index * tall
        out[at : at + tall, :rank] = edge[:, index * rank : (index + 1) * rank]
        out[at : at + tall, rank:] = jnp.zeros((tall, out.shape[1] - rank), jnp.bfloat16)


def attend_kernel(count):
    def body(core, q_mine, q_other, q_gain, cosine, sine, pooled, *refs):
        pieces = refs[:count]
        w_qn, w_qr, w_k, w_v, w_attn, w_pool, kept, outgoing = refs[count : count + 8]
        q_latent, latent, rope_twice, total = refs[count + 8 :]
        step = pl.program_id(0)
        rank = latent.shape[1]

        @pl.when(step == 0)
        def _():
            q_latent[...] = normed((q_mine[...] + q_other[...]).astype(jnp.bfloat16), q_gain[...])
            source = lax.broadcasted_iota(jnp.int32, (ROPE_DIM, 2 * ROPE_DIM), 0)
            target = lax.broadcasted_iota(jnp.int32, (ROPE_DIM, 2 * ROPE_DIM), 1)
            twice = jnp.where(target % ROPE_DIM == source, 1.0, 0.0).astype(jnp.bfloat16)
            at = 0
            for piece in pieces:
                rows = latent.shape[0] // count
                latent[at : at + rows, :] = piece[:rows, :rank]
                rope_twice[at : at + rows, :] = jnp.dot(
                    piece[:rows, rank:], twice, preferred_element_type=jnp.float32
                ).astype(jnp.bfloat16)
                at += rows
            total[...] = jnp.zeros(total.shape, jnp.float32)

        q_rows = q_latent[...]
        query = jnp.dot(q_rows, w_qn[...], preferred_element_type=jnp.float32).astype(jnp.bfloat16)
        pre = jnp.dot(q_rows, w_qr[...], preferred_element_type=jnp.float32).astype(jnp.bfloat16)
        rope = turned(pre, cosine[...], sine[...])
        keys = jnp.dot(latent[...], w_k[...], preferred_element_type=jnp.float32).astype(
            jnp.bfloat16
        )
        values = jnp.dot(latent[...], w_v[...], preferred_element_type=jnp.float32).astype(
            jnp.bfloat16
        )
        lane = lax.broadcasted_iota(jnp.int32, rope.shape, 1)
        factor = (NOPE_DIM + ROPE_DIM) ** (-0.5) * 1.4426950408889634
        features = []
        for head in range(2):
            own = (lane // ROPE_DIM) == head
            rope_head = jnp.where(own, rope.astype(jnp.float32), 0.0).astype(jnp.bfloat16)
            left = jnp.concatenate(
                [query[:, head * NOPE_DIM : (head + 1) * NOPE_DIM], rope_head], axis=1
            )
            right = jnp.concatenate(
                [keys[:, head * NOPE_DIM : (head + 1) * NOPE_DIM], rope_twice[...]], axis=1
            )
            scores = lax.dot_general(
                left, right, (((1,), (1,)), ((), ())), preferred_element_type=jnp.float32
            )
            top = jnp.max(scores, axis=1, keepdims=True)
            weights = jnp.exp2((scores - top) * factor)
            row_total = jnp.sum(weights, axis=1, keepdims=True)
            summed = jnp.dot(
                weights.astype(jnp.bfloat16),
                values[:, head * VALUE_DIM : (head + 1) * VALUE_DIM],
                preferred_element_type=jnp.float32,
            )
            features.append((summed / row_total).astype(jnp.bfloat16))
        attended = jnp.concatenate(features, axis=1)
        total[...] += jnp.dot(
            attended, w_attn[...], preferred_element_type=jnp.float32
        ) + jnp.dot(pooled[...], w_pool[...], preferred_element_type=jnp.float32)

        @pl.when(step == pl.num_programs(0) - 1)
        def _():
            half = kept.shape[0]
            kept[...] = total[pl.ds(pl.multiple_of(core[0] * half, 8), half), :]
            outgoing[...] = total[pl.ds(pl.multiple_of((1 - core[0]) * half, 8), half), :].astype(
                jnp.bfloat16
            )

    return body


def whole_call(kernel, shapes, scalars, *arrays):
    return pl.pallas_call(
        kernel,
        out_shape=shapes,
        in_specs=[pl.BlockSpec(memory_space=pltpu.SMEM)] * len(scalars)
        + [pl.BlockSpec(memory_space=pltpu.VMEM)] * len(arrays),
        out_specs=jax.tree.map(lambda _: pl.BlockSpec(memory_space=pltpu.VMEM), shapes),
    )(*scalars, *arrays)


def swap_tp(array):
    return lax.ppermute(array, "tp", [(0, 1), (1, 0)])


def flip_fs(array, bits):
    size = lax.axis_size("fs")
    return lax.ppermute(array, "fs", [(i, i ^ bits) for i in range(size)])


def row_parts(shard, core):
    rows = shard.shape[0] // 2
    mine = lax.dynamic_slice_in_dim(shard, core * rows, rows, 0)
    return (mine,) + tuple((flip_fs(mine, bits) for bits in range(1, lax.axis_size("fs"))))


def split_dot(hidden, parts, core):
    rows = parts[0].shape[0]
    here = lax.axis_index("fs")
    starts = (here ^ jnp.arange(len(parts), dtype=jnp.int32)) * (2 * rows) + core * rows
    shape = jax.ShapeDtypeStruct((hidden.shape[0], parts[0].shape[1]), jnp.float32)
    return whole_call(part_kernel, shape, (starts,), hidden, *parts)


def gather_sp(array, rows, rank):
    size = lax.axis_size("sp")
    here = lax.axis_index("sp")
    if size > 4:
        gathered = lax.all_gather(array, "sp", axis=0)
        pieces = (gathered[:, :rows].reshape(size * rows, array.shape[1]),)
        lower = lax.dynamic_index_in_dim(gathered, jnp.maximum(here - 1, 0), 0, False)
        upper = lax.dynamic_index_in_dim(gathered, jnp.minimum(here + 1, size - 1), 0, False)
    else:
        pieces = [array]
        for shift in range(1, size):
            ring = [(i, (i + shift) % size) for i in range(size)]
            pieces.append(lax.ppermute(array, "sp", ring))
        lower, upper = pieces[1 % size], pieces[size - 1]

    def edges(piece, start):
        tall = 2 * rim_width
        count = (piece.shape[0] - rows) // tall
        parts = [
            piece[rows + i * tall + start : rows + i * tall + start + rim_width, :rank]
            for i in range(count)
        ]
        return jnp.concatenate(parts, axis=1)

    before = jnp.where(here > 0, edges(lower, rim_width), 0)
    after = jnp.where(here < size - 1, edges(upper, 0), 0)
    return tuple(pieces), before, after


def on_device(
    tokens,
    norm_gain,
    w_q_down,
    q_gain,
    w_q_nope,
    w_q_rope,
    w_kv_down,
    kv_gain,
    w_k_up,
    w_v_up,
    w_k_rope,
    w_pool_in,
    w_pool_mix,
    w_out_attn,
    w_out_pool,
):
    core = lax.axis_index("tp")
    core_ref = core.astype(jnp.int32).reshape(1)
    own_rows = tokens[0]
    other_rows, other_gain = swap_tp(own_rows), swap_tp(norm_gain)
    kv_parts = row_parts(w_kv_down, core)
    q_parts = row_parts(w_q_down, core)
    local_rows = own_rows.shape[0]
    length = local_rows * lax.axis_size("sp")
    position = lax.axis_index("sp") * local_rows + jnp.arange(local_rows, dtype=jnp.int32)
    cosine, sine = position_tables(position, 2 * ROPE_DIM)
    width = 2 * own_rows.shape[1]
    hidden, pool_in, key_rope = whole_call(
        front_kernel,
        (
            jax.ShapeDtypeStruct((local_rows, width), jnp.bfloat16),
            jax.ShapeDtypeStruct((local_rows, w_pool_in.shape[1]), jnp.bfloat16),
            jax.ShapeDtypeStruct((local_rows, ROPE_DIM), jnp.bfloat16),
        ),
        (core_ref,),
        own_rows,
        other_rows,
        norm_gain,
        other_gain,
        w_pool_in,
        w_k_rope.T,
        cosine,
        sine,
    )
    kv_share = split_dot(hidden, kv_parts, core)
    kv_rank = kv_share.shape[1]
    tail = pool_in.shape[1] // kv_rank * 2 * rim_width
    shared = whole_call(
        latent_kernel,
        jax.ShapeDtypeStruct((local_rows + tail, kv_rank + ROPE_DIM), jnp.bfloat16),
        (),
        kv_share,
        swap_tp(kv_share),
        kv_gain[None],
        key_rope,
        pool_in,
    )
    pieces, rim_before, rim_after = gather_sp(shared, local_rows, kv_rank)
    late_hidden, _ = lax.optimization_barrier((hidden, shared))
    q_share = split_dot(late_hidden, q_parts, core)
    q_other = swap_tp(q_share)
    groups_dev = pool_in.shape[1] // POOL_GROUP
    group_id = lax.axis_index("tp") * groups_dev + jnp.arange(groups_dev, dtype=jnp.int32)
    window = jnp.zeros((groups_dev,), jnp.int32)
    for group_index, window_size in enumerate(window_sizes):
        window = window + jnp.where(group_id == group_index, window_size, 0).astype(jnp.int32)
    window = jnp.repeat(window, POOL_GROUP)
    before = window // 2
    window_after = window - before
    padded = jnp.concatenate([rim_before, pool_in, rim_after], axis=0)
    padded_wide = padded.astype(jnp.float32)
    window_sum = jnp.zeros(pool_in.shape, jnp.float32)
    for offset in range(-rim_width, rim_width):
        inside = ((offset >= -before) & (offset < window_after)).astype(jnp.float32)
        window_sum = (
            window_sum + padded_wide[rim_width + offset : rim_width + offset + local_rows] * inside
        )
    low_edge = jnp.clip(position[:, None] - before[None, :], 0, length)
    high_edge = jnp.clip(position[:, None] + window_after[None, :], 0, length)
    window_mean = (window_sum / (high_edge - low_edge).astype(jnp.float32)).astype(jnp.bfloat16)
    spread = (window_mean - pool_in).reshape(local_rows, groups_dev, POOL_GROUP)
    mixing = lax.dynamic_slice_in_dim(w_pool_mix, lax.axis_index("tp") * groups_dev, groups_dev, 0)
    pooled = jnp.einsum("tgc,gce->tge", spread, mixing, preferred_element_type=jnp.float32).astype(
        jnp.bfloat16
    )
    pooled = pooled.reshape(local_rows, groups_dev * POOL_GROUP)
    steps = w_q_nope.shape[1] // (2 * NOPE_DIM)
    q_rank, features = q_share.shape[1], w_out_attn.shape[1]
    half = local_rows // 2
    pool_rows = pooled.shape[1] // steps

    def fixed(array):
        return pl.BlockSpec(array.shape, lambda p: (0, 0))

    def by_column(array):
        return pl.BlockSpec((array.shape[0], array.shape[1] // steps), lambda p: (0, p))

    def by_row(array):
        return pl.BlockSpec((array.shape[0] // steps, array.shape[1]), lambda p: (p, 0))

    kept, outgoing = pl.pallas_call(
        attend_kernel(len(pieces)),
        grid=(steps,),
        in_specs=[
            pl.BlockSpec(memory_space=pltpu.SMEM),
            fixed(q_share),
            fixed(q_other),
            fixed(q_gain[None]),
            fixed(cosine),
            fixed(sine),
            by_column(pooled),
        ]
        + [fixed(piece) for piece in pieces]
        + [by_column(w) for w in (w_q_nope, w_q_rope, w_k_up, w_v_up)]
        + [by_row(w_out_attn), by_row(w_out_pool)],
        out_specs=(
            pl.BlockSpec((half, features), lambda p: (0, 0)),
            pl.BlockSpec((half, features), lambda p: (0, 0)),
        ),
        out_shape=(
            jax.ShapeDtypeStruct((half, features), jnp.float32),
            jax.ShapeDtypeStruct((half, features), jnp.bfloat16),
        ),
        scratch_shapes=[
            pltpu.VMEM((local_rows, q_rank), jnp.bfloat16),
            pltpu.VMEM((length, kv_rank), jnp.bfloat16),
            pltpu.VMEM((length, 2 * ROPE_DIM), jnp.bfloat16),
            pltpu.VMEM((local_rows, features), jnp.float32),
        ],
        compiler_params=pltpu.CompilerParams(dimension_semantics=("arbitrary",)),
    )(
        core_ref,
        q_share,
        q_other,
        q_gain[None],
        cosine,
        sine,
        pooled,
        *pieces,
        w_q_nope,
        w_q_rope,
        w_k_up,
        w_v_up,
        w_out_attn,
        w_out_pool,
    )
    incoming = swap_tp(outgoing)
    out_share = (kept + incoming.astype(jnp.float32)).astype(jnp.bfloat16)
    return out_share[None]


def solution(mesh):
    placed = (
        P("fs", "sp", "tp"),
        P("tp"),
        P("fs", None),
        P(),
        P(None, "tp"),
        P(None, "tp"),
        P("fs", None),
        P(),
        P(None, "tp"),
        P(None, "tp"),
        P(),
        P(None, "tp"),
        P(),
        P("tp", None),
        P("tp", None),
    )
    return jax.shard_map(
        on_device,
        mesh=mesh,
        in_specs=placed,
        out_specs=P("fs", ("sp", "tp"), None),
        check_vma=False,
    )
```
